32 devices in a mesh: fs: 8 (over z, y), tp: 4 (over x, core).
Axes of the slice: x: 2, y: 2, z: 4, core: 2. Of those that a mesh axis runs over, the one named last changes fastest.
Arguments:
- rnn_out: bfloat16 [6144, 1536], P('fs', 'tp'), may hold values from -6 to 6
- out_grad: bfloat16 [6144, 2048], P('fs', 'tp'), may hold values from -0.109375 to 0.109375
- weight: float32 [2048, 1536], P('fs', 'tp'), may hold values from -0.15625 to 0.15625
- left_root: bfloat16 [4, 2048, 2048], P('tp', 'fs'), as said below
- right_root: bfloat16 [4, 384, 384], P('tp'), as said below
- left_stat: float32 [4, 2048, 2048], P('tp', 'fs'), may hold values from -4 to 4
- right_stat: float32 [4, 384, 384], P('tp', 'fs'), may hold values from -4 to 4
Outputs:
- new_weight: float32 [2048, 1536], P('fs', 'tp')
- step: float32 [2048, 1536], P('fs', 'tp')
- left_new: float32 [4, 2048, 2048], P('tp', 'fs')
- right_new: float32 [4, 384, 384], P('tp', 'fs')
- weight_copy: bfloat16 [2048, 1536], P(None, 'tp')
The draws below stay inside these ranges and needn't reach their ends.
Inputs may be any that keep to these rules, and one draw needn't show every extreme that they name: `left_root`: each block is symmetric. `right_root`: each block is symmetric.
All inputs are finite; a program needn't handle non-finite values.
Results may differ from the reference program's by a relative error of at most 0.0049.
Values may be sent and summed in bfloat16 or wider, within the bound.
A program may use at most 64 MiB of HBM per device.

```python
import jax
import jax.numpy as jnp

D = 2048
R = 1536
TOKENS = 6144
NB = 4
RB = 384


def symmetric_root(key, width):
    noise = jax.random.normal(key, (NB, width, width), jnp.float32)
    mixed = (noise + jnp.swapaxes(noise, 1, 2)) * (0.5 / (2.0 * width) ** 0.5)
    matrix = jnp.eye(width, dtype=jnp.float32)[None] + mixed
    return matrix


def draw_left_root(key, part):
    return symmetric_root(jax.random.fold_in(key, 11), D).astype(jnp.bfloat16)


def draw_right_root(key, part):
    return symmetric_root(jax.random.fold_in(key, 23), RB).astype(jnp.bfloat16)


def spiked(values, own_key, source, target, blocks, factor):
    def block_of(position):
        return (jnp.arange(values.shape[position]) // (values.shape[position] // blocks)).reshape((-1,) + (1,) * (values.ndim - 1 - position))

    first = jax.random.permutation(own_key, blocks)[block_of(target)]
    second = (block_of(target) + blocks // 2) % blocks
    return jnp.where((block_of(source) == first) | (block_of(source) == second), factor * values, values)


def block_levels(rng, shape, cuts, smallest, top_value):
    def one(position, shards_of):
        heights = jax.random.uniform(jax.random.fold_in(jax.random.fold_in(rng, 6), position), (shards_of,), jnp.float32, smallest / len(cuts), top_value / len(cuts))
        return jnp.repeat(jnp.exp(heights), shape[position] // shards_of).reshape((-1,) + (1,) * (len(shape) - position - 1))

    factor_of = one(*cuts[0])
    for cut in cuts[1:]:
        factor_of = factor_of * one(*cut)
    return factor_of


def normal_values(own_key, extent, scale, most, split=(), kind=jnp.bfloat16):
    result = scale * jax.random.normal(own_key, extent, jnp.float32)
    if split:
        result = result * block_levels(own_key, extent, split, -0.22, 0.18)
    return jnp.clip(result, -most, most).astype(kind)


def heavy_noise(rng, extent, scale, reach, pieces, heavy, kind=jnp.bfloat16):
    entries = scale * jax.random.normal(rng, extent, jnp.float32)
    if pieces:
        entries = entries * block_levels(rng, extent, pieces, -0.22, 0.18)
    return jnp.clip(spiked(entries, jax.random.fold_in(rng, 3), *heavy), -reach, reach).astype(kind)


def setup_inputs(seed: int = 0) -> dict:
    streams_of = jax.random.split(jax.random.key(seed), 8)
    rnn_out = normal_values(streams_of[0], (TOKENS, R), 1.0, 6.0, ((0, 8), (1, 4)))
    out_grad = heavy_noise(streams_of[1], (TOKENS, D), (1.0 / TOKENS ** 0.5), 0.109375, ((0, 8), (1, 4)), (0, 1, 8, 2.0))
    weight = normal_values(streams_of[2], (D, R), R ** -0.5, 0.15625, ((0, 8), (1, 4)), jnp.float32)
    left_root = draw_left_root(jax.random.fold_in(streams_of[7], 71), 0)
    right_root = draw_right_root(jax.random.fold_in(streams_of[7], 71), 0)
    left_stat = normal_values(streams_of[5], (NB, D, D), 0.5, 4.0, ((0, 4), (1, 8)), jnp.float32)
    right_stat = normal_values(streams_of[6], (NB, RB, RB), 0.5, 4.0, ((0, 4), (1, 8)), jnp.float32)
    return dict(rnn_out=rnn_out, out_grad=out_grad, weight=weight, left_root=left_root, right_root=right_root, left_stat=left_stat, right_stat=right_stat)


decay_rate = 0.8
step_size = 0.005

def reference(rnn_out, out_grad, weight, left_root, right_root, left_stat, right_stat):
    grad = jnp.dot(out_grad.T, rnn_out, preferred_element_type=jnp.float32)
    grad_low = grad.astype(jnp.bfloat16)
    grad_square = jnp.sum(grad * grad)
    lefts = []
    rights = []
    updates = []
    for index in range(NB):
        column = grad_low[:, index * RB:(index + 1) * RB]
        outer = jnp.dot(column, column.T, preferred_element_type=jnp.float32) / RB
        inner = jnp.dot(column.T, column, preferred_element_type=jnp.float32) / D
        lefts.append(decay_rate * left_stat[index] + (1.0 - decay_rate) * outer)
        rights.append(decay_rate * right_stat[index] + (1.0 - decay_rate) * inner)
        applied = jnp.dot(left_root[index], column, preferred_element_type=jnp.float32).astype(jnp.bfloat16)
        updates.append(jnp.dot(applied, right_root[index], preferred_element_type=jnp.float32))
    update = jnp.concatenate(updates, axis=1)
    scale = jnp.sqrt(grad_square + 1.0) / jnp.sqrt(jnp.sum(update * update) + 1.0)
    step = scale * update
    new_weight = weight - step_size * step
    return (new_weight, step, jnp.stack(lefts), jnp.stack(rights), new_weight.astype(jnp.bfloat16))
```

```python
import functools

import jax
import jax.numpy as jnp
from jax import lax
from jax.experimental import pallas as pl
from jax.experimental.pallas import tpu as pltpu
from jax.sharding import PartitionSpec as P

decay_rate = 0.8
step_size = 0.005
MESH = pl.DeviceIdType.MESH
bf16, f32 = jnp.bfloat16, jnp.float32


def loop(count, step):
    if count <= 8:
        for k in range(count):
            step(k)
    else:
        lax.fori_loop(0, count, lambda k, _: (step(k), 0)[1], 0)


def kernel(
    nfs, ntp,
    og, rnn, w, lroot, rroot, lstat, rstat,
    new_w, step, lnew, rnew, wcopy,
    ogb, rnnb, wb, lrootb, rrootb, lstatb, rstatb,
    part, ysend, yrecv, zsend, zrecv, mine, full, wfull,
    newb, stepb, rnewb, tpred, fsred,
    lsem, osem, ts, tr, ys, yr, zs, zr,
    gzs, gzr, gys, gyr, wzs, wzr, wys, wyr, rts, rtr, rfs, rfr,
):
    f = lax.axis_index("fs")
    t = lax.axis_index("tp")
    y = lax.rem(f, 2)
    z = lax.div(f, 2)
    nz = nfs // 2
    pair = f + 1 - 2 * y
    rows, chans = w.shape
    dl = og.shape[1]
    cpb = dl // rows
    half = cpb // 2
    width = lroot.shape[2]
    aligned = cpb == 2 and rows % 128 == 0

    def remote(src, dst, s, r, ff, tt):
        return pltpu.make_async_remote_copy(
            src_ref=src, dst_ref=dst, send_sem=s, recv_sem=r,
            device_id=(ff, tt), device_id_type=MESH,
        )

    def chunk(k):
        return pl.ds(pl.multiple_of(k * rows, rows), rows)

    og_in = pltpu.make_async_copy(og, ogb.at[t], lsem.at[0])
    og_in.start()
    loads = []
    for i, (a, b) in enumerate(
        [(rnn, rnnb), (lroot.at[0], lrootb), (rroot.at[0], rrootb), (w, wb),
         (lstat.at[0], lstatb), (rstat.at[0], rstatb)]
    ):
        c = pltpu.make_async_copy(a, b, lsem.at[i + 1])
        c.start()
        loads.append(c)

    barrier = pltpu.get_barrier_semaphore()
    for k in range(1, ntp):
        pl.semaphore_signal(barrier, inc=1, device_id=(f, t ^ k), device_id_type=MESH)

    def greet(k):
        pl.semaphore_signal(
            barrier, inc=1, device_id=(lax.rem(f + k + 1, nfs), t), device_id_type=MESH
        )

    loop(nfs - 1, greet)
    pl.semaphore_wait(barrier, ntp - 1 + nfs - 1)
    og_in.wait()

    pieces = 2 if aligned else 1
    pc = dl // pieces

    def piece_of(s, p):
        if pieces == 1:
            return ogb.at[s]
        q = (1 - y) if p == 0 else y
        return ogb.at[s, :, pl.ds(pl.multiple_of(q * pc, pc), pc)]

    def own_copy(k, p):
        return remote(piece_of(t, p), piece_of(t, p), ts.at[k, p], tr.at[t, p], f, t ^ k)

    def forward_copy(k, p):
        b = t ^ k
        return remote(piece_of(b, p), piece_of(b, p), ts.at[ntp + k, p], tr.at[b, p], f, t ^ 1)

    def arrival(k, p):
        b = t ^ k
        return remote(piece_of(b, p), piece_of(b, p), ts.at[0, 0], tr.at[b, p], f, t ^ 1)

    far = [k for k in range(2, ntp, 2)]
    for p in range(pieces):
        for k in far:
            own_copy(k, p).start()
    if ntp > 1:
        for p in range(pieces):
            own_copy(1, p).start()

    def y_copy(s):
        return remote(ysend.at[s], yrecv.at[s], ys.at[s], yr.at[s], pair, t)

    def product(s, p):
        return lax.dot_general(
            piece_of(s, p)[...], rnnb[...], (((0,), (0,)), ((), ())),
            preferred_element_type=f32,
        )

    def ready(k, p):
        if k:
            arrival(k, p).wait_recv()
            if k % 2 == 0:
                forward_copy(k, p).start()

    def do_block(k):
        s = t ^ k
        if aligned:
            ready(k, 0)
            ysend[s, 0] = product(s, 0).astype(bf16)
            y_copy(s).start()
            ready(k, 1)
            part[s, 0] = product(s, 1)
        else:
            ready(k, 0)
            out = product(s, 0).reshape(half, 2, rows, chans)
            odd, even = out[:, 1], out[:, 0]
            low = y == 0
            ysend[s] = jnp.where(low, odd, even).astype(bf16)
            part[s] = jnp.where(low, even, odd)
            y_copy(s).start()

    def z_copy(zp):
        return remote(zsend.at[zp], zrecv.at[z], zs.at[zp], zr.at[z], 2 * zp + y, t)

    def pass_on(k):
        s = t ^ k
        y_copy(s).wait_recv()

        def one(c):
            zp = s * half + c
            total = part[s, c] + yrecv[s, c].astype(f32)

            @pl.when(zp == z)
            def _():
                mine[...] = total

            @pl.when(zp != z)
            def _():
                zsend[zp] = total.astype(bf16)
                z_copy(zp).start()

        loop(half, one)

    loads[0].wait()
    order = list(range(ntp))
    for i, k in enumerate(order):
        do_block(k)
        if i >= 1:
            pass_on(order[i - 1])
    pass_on(order[-1])

    def take(k):
        src = lax.rem(z + k + 1, nz)
        remote(zsend.at[src], zrecv.at[src], zs.at[src], zr.at[src], 2 * src + y, t).wait_recv()
        mine[...] += zrecv[src].astype(f32)

    loop(nz - 1, take)
    grad = mine[...]
    full[chunk(f), :] = grad.astype(bf16)

    def gather_start(buf, szs, szr, sys, syr):
        def z_send(k):
            zp = lax.rem(z + k + 1, nz)
            remote(buf.at[chunk(f)], buf.at[chunk(f)], szs.at[k], szr.at[z], 2 * zp + y, t).start()

        remote(buf.at[chunk(f)], buf.at[chunk(f)], sys.at[z], syr.at[z], pair, t).start()
        loop(nz - 1, z_send)

    def gather_forward(buf, szs, szr, sys, syr, k):
        zp = lax.rem(z + k + 1, nz)
        c = chunk(2 * zp + y)
        remote(buf.at[c], buf.at[c], szs.at[0], szr.at[zp], 2 * zp + y, t).wait_recv()
        remote(buf.at[c], buf.at[c], sys.at[zp], syr.at[zp], pair, t).start()

    def gather_pair(buf, szs, szr, sys, syr, zi):
        c = chunk(2 * zi + 1 - y)
        remote(buf.at[c], buf.at[c], sys.at[zi], syr.at[zi], pair, t).wait_recv()

    def gather_drain(buf, szs, szr, sys, syr):
        def z_drain(k):
            zp = lax.rem(z + k + 1, nz)
            remote(buf.at[chunk(f)], buf.at[chunk(f)], szs.at[k], szr.at[z], 2 * zp + y, t).wait_send()

        def y_drain(zi):
            c = chunk(2 * zi + y)
            remote(buf.at[c], buf.at[c], sys.at[zi], syr.at[zi], pair, t).wait_send()

        loop(nz - 1, z_drain)
        loop(nz, y_drain)

    ga = (full, gzs, gzr, gys, gyr)
    gather_start(*ga)
    grad_square = jnp.sum(grad * grad)
    loop(nz - 1, functools.partial(gather_forward, *ga))
    for c in loads[1:]:
        c.wait()
    loop(nz, functools.partial(gather_pair, *ga))

    left_sum = jnp.dot(lrootb[...], full[...], preferred_element_type=f32)
    update = jnp.dot(left_sum.astype(bf16), rrootb[...], preferred_element_type=f32)
    update_square = jnp.sum(update * update)
    stepb[...] = update

    line = lax.broadcasted_iota(jnp.int32, (8, 128), 0)
    tpred[t] = jnp.where(line == 0, grad_square, update_square)

    def tp_red(k):
        return remote(tpred.at[t], tpred.at[t], rts.at[k], rtr.at[t], f, t ^ k)

    for k in range(1, ntp):
        tp_red(k).start()
    rr = rstat.shape[1]
    pick = lax.broadcasted_iota(jnp.int32, (rr, chans), 1) == (
        lax.broadcasted_iota(jnp.int32, (rr, chans), 0) + f * rr
    )
    own_columns = lax.dot_general(
        jnp.where(pick, 1.0, 0.0).astype(bf16), full[...], (((1,), (1,)), ((), ())),
        preferred_element_type=f32,
    ).astype(bf16)
    right_sum = jnp.dot(own_columns, full[...], preferred_element_type=f32)
    rnewb[...] = decay_rate * rstatb[...] + (1.0 - decay_rate) * (right_sum / width)
    right_out = pltpu.make_async_copy(rnewb, rnew.at[0], osem.at[0])
    right_out.start()
    for k in range(1, ntp):
        b = t ^ k
        remote(tpred.at[b], tpred.at[b], rts.at[k], rtr.at[b], f, b).wait_recv()
    fsred[f] = jnp.sum(tpred[...], axis=0)

    def fs_red(k):
        peer = lax.rem(f + k + 1, nfs)
        return remote(fsred.at[f], fsred.at[f], rfs.at[k], rfr.at[f], peer, t)

    loop(nfs - 1, lambda k: fs_red(k).start())

    outer = lax.dot_general(
        full[chunk(f), :], full[...], (((1,), (1,)), ((), ())), preferred_element_type=f32
    )
    lstatb[...] = decay_rate * lstatb[...] + (1.0 - decay_rate) * (outer / chans)
    left_out = pltpu.make_async_copy(lstatb, lnew.at[0], osem.at[1])
    left_out.start()

    def fs_take(k):
        peer = lax.rem(f + k + 1, nfs)
        remote(fsred.at[peer], fsred.at[peer], rfs.at[k], rfr.at[peer], peer, t).wait_recv()

    loop(nfs - 1, fs_take)
    totals = jnp.sum(fsred[...], axis=0)
    scale = jnp.sqrt(totals[0:1, 0:1] + 1.0) / jnp.sqrt(totals[1:2, 0:1] + 1.0)
    stepv = scale * stepb[...]
    stepb[...] = stepv
    new = wb[...] - step_size * stepv
    newb[...] = new
    wfull[chunk(f), :] = new.astype(bf16)
    wa = (wfull, wzs, wzr, wys, wyr)
    gather_start(*wa)
    step_out = pltpu.make_async_copy(stepb, step, osem.at[2])
    step_out.start()
    new_out = pltpu.make_async_copy(newb, new_w, osem.at[3])
    new_out.start()

    for p in range(pieces):
        for k in far:
            own_copy(k, p).wait_send()
            forward_copy(k, p).wait_send()
        if ntp > 1:
            own_copy(1, p).wait_send()
    for s in range(ntp):
        y_copy(s).wait_send()

    def z_drain(k):
        z_copy(lax.rem(z + k + 1, nz)).wait_send()

    loop(nz - 1, z_drain)
    gather_drain(*ga)
    for k in range(1, ntp):
        tp_red(k).wait_send()
    loop(nfs - 1, lambda k: fs_red(k).wait_send())

    loop(nz - 1, functools.partial(gather_forward, *wa))
    loop(nz, functools.partial(gather_pair, *wa))
    copy_out = pltpu.make_async_copy(wfull, wcopy, osem.at[4])
    copy_out.start()
    gather_drain(*wa)
    for c in (right_out, left_out, step_out, new_out, copy_out):
        c.wait()


def body(nfs, ntp, rnn_out, out_grad, weight, left_root, right_root, left_stat, right_stat):
    rows, chans = weight.shape
    tokens, dl = out_grad.shape
    width = left_root.shape[2]
    rr = right_stat.shape[1]
    nz = nfs // 2
    half = dl // rows // 2
    pieces = 2 if (half == 1 and rows % 128 == 0) else 1
    dma = pltpu.SemaphoreType.DMA
    hbm = pl.BlockSpec(memory_space=pl.ANY)
    V = pltpu.VMEM
    return pl.pallas_call(
        functools.partial(kernel, nfs, ntp),
        out_shape=(
            jax.ShapeDtypeStruct(weight.shape, f32),
            jax.ShapeDtypeStruct(weight.shape, f32),
            jax.ShapeDtypeStruct(left_stat.shape, f32),
            jax.ShapeDtypeStruct(right_stat.shape, f32),
            jax.ShapeDtypeStruct((width, chans), bf16),
        ),
        in_specs=[hbm] * 7,
        out_specs=(hbm,) * 5,
        scratch_shapes=[
            V((ntp, tokens, dl), bf16),
            V((tokens, chans), bf16),
            V((rows, chans), f32),
            V((rows, width), bf16),
            V((chans, chans), bf16),
            V((rows, width), f32),
            V((rr, chans), f32),
            V((ntp, half, rows, chans), f32),
            V((ntp, half, rows, chans), bf16),
            V((ntp, half, rows, chans), bf16),
            V((nz, rows, chans), bf16),
            V((nz, rows, chans), bf16),
            V((rows, chans), f32),
            V((width, chans), bf16),
            V((width, chans), bf16),
            V((rows, chans), f32),
            V((rows, chans), f32),
            V((rr, chans), f32),
            V((ntp, 8, 128), f32),
            V((nfs, 8, 128), f32),
            dma((7,)),
            dma((5,)),
            dma((2 * ntp, pieces)),
            dma((ntp, pieces)),
            dma((ntp,)),
            dma((ntp,)),
            dma((nz,)),
            dma((nz,)),
            dma((nz,)), dma((nz,)), dma((nz,)), dma((nz,)),
            dma((nz,)), dma((nz,)), dma((nz,)), dma((nz,)),
            dma((ntp,)), dma((ntp,)),
            dma((nfs,)), dma((nfs,)),
        ],
        compiler_params=pltpu.CompilerParams(
            collective_id=0, has_side_effects=True, vmem_limit_bytes=60000 * 1024
        ),
    )(out_grad, rnn_out, weight, left_root, right_root, left_stat, right_stat)


def solution(mesh):
    placed = (
        P("fs", "tp"),
        P("fs", "tp"),
        P("fs", "tp"),
        P("tp", "fs", None),
        P("tp", None, None),
        P("tp", "fs", None),
        P("tp", "fs", None),
    )
    return jax.shard_map(
        functools.partial(body, mesh.shape["fs"], mesh.shape["tp"]),
        mesh=mesh,
        in_specs=placed,
        out_specs=(
            P("fs", "tp"),
            P("fs", "tp"),
            P("tp", "fs", None),
            P("tp", "fs", None),
            P(None, "tp"),
        ),
        check_vma=False,
    )
```

```python
import functools

import jax
import jax.numpy as jnp
from jax import lax
from jax.experimental import pallas as pl
from jax.experimental.pallas import tpu as pltpu
from jax.sharding import PartitionSpec as P

decay_rate = 0.8
step_size = 0.005
MESH = pl.DeviceIdType.MESH
bf16, f32 = jnp.bfloat16, jnp.float32


def loop(count, step):
    if count <= 32:
        for k in range(count):
            step(k)
    else:
        lax.fori_loop(0, count, lambda k, _: (step(k), 0)[1], 0)


def kernel(
    nfs, ntp,
    og, rnn, w, lroot, rroot, lstat, rstat,
    new_w, step, lnew, rnew, wcopy,
    ogb, rnnb, wb, lrootb, rrootb, lstatb, rstatb,
    part, ysend, yrecv, zsend, zrecv, mine, full, tpred, fsred,
    lsem, ts, tr, ys, yr, zs, zr,
    gzs, gzr, gys, gyr, wzs, wzr, wys, wyr, rts, rtr, rfs, rfr,
):
    f = lax.axis_index("fs")
    t = lax.axis_index("tp")
    y = lax.rem(f, 2)
    z = lax.div(f, 2)
    nz = nfs // 2
    pair = f + 1 - 2 * y
    rows, chans = w.shape
    dl = og.shape[1]
    cpb = dl // rows
    half = cpb // 2
    width = lroot.shape[2]
    np_ = 4 if rows % 64 == 0 else 1
    pr = rows // np_
    aligned = cpb == 2 and rows % 128 == 0

    def remote(src, dst, s, r, ff, tt):
        return pltpu.make_async_remote_copy(
            src_ref=src, dst_ref=dst, send_sem=s, recv_sem=r,
            device_id=(ff, tt), device_id_type=MESH,
        )

    def chunk(k):
        return pl.ds(pl.multiple_of(k * rows, rows), rows)

    og_in = pltpu.make_async_copy(og, ogb.at[t], lsem.at[0])
    og_in.start()
    loads = []
    for i, (a, b) in enumerate(
        [(rnn, rnnb), (lroot.at[0], lrootb), (rroot.at[0], rrootb), (w, wb),
         (lstat.at[0], lstatb), (rstat.at[0], rstatb)]
    ):
        c = pltpu.make_async_copy(a, b, lsem.at[i + 1])
        c.start()
        loads.append(c)

    barrier = pltpu.get_barrier_semaphore()
    for k in range(1, ntp):
        pl.semaphore_signal(barrier, inc=1, device_id=(f, t ^ k), device_id_type=MESH)

    def greet(k):
        pl.semaphore_signal(
            barrier, inc=1, device_id=(lax.rem(f + k + 1, nfs), t), device_id_type=MESH
        )

    loop(nfs - 1, greet)
    pl.semaphore_wait(barrier, ntp - 1 + nfs - 1)
    og_in.wait()

    pieces = 2 if aligned else 1
    pc = dl // pieces

    def piece_of(s, p):
        if pieces == 1:
            return ogb.at[s]
        q = (1 - y) if p == 0 else y
        return ogb.at[s, :, pl.ds(pl.multiple_of(q * pc, pc), pc)]

    def own_copy(k, p):
        return remote(piece_of(t, p), piece_of(t, p), ts.at[k, p], tr.at[t, p], f, t ^ k)

    def forward_copy(k, p):
        b = t ^ k
        return remote(piece_of(b, p), piece_of(b, p), ts.at[ntp + k, p], tr.at[b, p], f, t ^ 1)

    def arrival(k, p):
        b = t ^ k
        return remote(piece_of(b, p), piece_of(b, p), ts.at[0, 0], tr.at[b, p], f, t ^ 1)

    far = [k for k in range(2, ntp, 2)]
    for p in range(pieces):
        for k in far:
            own_copy(k, p).start()
    if ntp > 1:
        for p in range(pieces):
            own_copy(1, p).start()

    def y_copy(s):
        return remote(ysend.at[s], yrecv.at[s], ys.at[s], yr.at[s], pair, t)

    def product(s, p):
        return lax.dot_general(
            piece_of(s, p)[...], rnnb[...], (((0,), (0,)), ((), ())),
            preferred_element_type=f32,
        )

    def ready(k, p):
        if k:
            arrival(k, p).wait_recv()
            if k % 2 == 0:
                forward_copy(k, p).start()

    def do_block(k):
        s = t ^ k
        if aligned:
            ready(k, 0)
            ysend[s, 0] = product(s, 0).astype(bf16)
            y_copy(s).start()
            ready(k, 1)
            part[s, 0] = product(s, 1)
        else:
            ready(k, 0)
            out = product(s, 0).reshape(half, 2, rows, chans)
            odd, even = out[:, 1], out[:, 0]
            low = y == 0
            ysend[s] = jnp.where(low, odd, even).astype(bf16)
            part[s] = jnp.where(low, even, odd)
            y_copy(s).start()

    def z_copy(zp):
        return remote(zsend.at[zp], zrecv.at[z], zs.at[zp], zr.at[z], 2 * zp + y, t)

    def pass_on(k):
        s = t ^ k
        y_copy(s).wait_recv()

        def one(c):
            zp = s * half + c
            total = part[s, c] + yrecv[s, c].astype(f32)

            @pl.when(zp == z)
            def _():
                mine[...] = total

            @pl.when(zp != z)
            def _():
                zsend[zp] = total.astype(bf16)
                z_copy(zp).start()

        loop(half, one)

    loads[0].wait()
    order = list(range(ntp))
    for i, k in enumerate(order):
        do_block(k)
        if i >= 1:
            pass_on(order[i - 1])
    pass_on(order[-1])

    def take(k):
        src = lax.rem(z + k + 1, nz)
        remote(zsend.at[src], zrecv.at[src], zs.at[src], zr.at[src], 2 * src + y, t).wait_recv()
        mine[...] += zrecv[src].astype(f32)

    loop(nz - 1, take)
    grad = mine[...]
    full[chunk(f), :] = grad.astype(bf16)

    def piece(k, p):
        return pl.ds(pl.multiple_of(k * rows + p * pr, pr), pr)

    def hop(g, d, zi, p):
        buf, zsend_s, zrecv_s = g[0], g[1], g[2]
        c = piece(2 * zi + y, p)
        to = z + 1 - 2 * d
        return remote(buf.at[c], buf.at[c], zsend_s.at[d, zi * np_ + p],
                      zrecv_s.at[zi * np_ + p], 2 * to + y, t)

    def across(g, zi, p, side):
        buf, ysend_s, yrecv_s = g[0], g[3], g[4]
        c = piece(2 * zi + side, p)
        return remote(buf.at[c], buf.at[c], ysend_s.at[zi * np_ + p],
                      yrecv_s.at[zi * np_ + p], pair, t)

    def gather_start(g):
        for p in range(np_):
            @pl.when(z < nz - 1)
            def _():
                hop(g, 0, z, p).start()

            @pl.when(z > 0)
            def _():
                hop(g, 1, z, p).start()

            across(g, z, p, y).start()

    def gather_relay(g):
        def one(i):
            d, p = i // np_ + 1, i % np_

            @pl.when(z - d >= 0)
            def _():
                hop(g, 0, z - d, p).wait_recv()

                @pl.when(z < nz - 1)
                def _():
                    hop(g, 0, z - d, p).start()

                across(g, z - d, p, y).start()

            @pl.when(z + d <= nz - 1)
            def _():
                hop(g, 1, z + d, p).wait_recv()

                @pl.when(z > 0)
                def _():
                    hop(g, 1, z + d, p).start()

                across(g, z + d, p, y).start()

        loop((nz - 1) * np_, one)

    def gather_pair(g, zi):
        for p in range(np_):
            across(g, zi, p, 1 - y).wait_recv()

    def gather_drain(g):
        def one(i):
            zi, p = i // np_, i % np_

            @pl.when((zi <= z) & (z < nz - 1))
            def _():
                hop(g, 0, zi, p).wait_send()

            @pl.when((zi >= z) & (z > 0))
            def _():
                hop(g, 1, zi, p).wait_send()

            across(g, zi, p, y).wait_send()

        loop(nz * np_, one)

    ga = (full, gzs, gzr, gys, gyr)
    gather_start(ga)
    grad_square = jnp.sum(grad * grad)
    gather_relay(ga)
    for c in loads[1:]:
        c.wait()
    loop(nz, functools.partial(gather_pair, ga))

    left_sum = jnp.dot(lrootb[...], full[...], preferred_element_type=f32)
    update = jnp.dot(left_sum.astype(bf16), rrootb[...], preferred_element_type=f32)
    update_square = jnp.sum(update * update)
    step[...] = update

    line = lax.broadcasted_iota(jnp.int32, (8, 128), 0)
    tpred[t] = jnp.where(line == 0, grad_square, update_square)

    def tp_red(k):
        return remote(tpred.at[t], tpred.at[t], rts.at[k], rtr.at[t], f, t ^ k)

    for k in range(1, ntp):
        tp_red(k).start()
    rr = rstat.shape[1]
    pick = lax.broadcasted_iota(jnp.int32, (rr, chans), 1) == (
        lax.broadcasted_iota(jnp.int32, (rr, chans), 0) + f * rr
    )
    own_columns = lax.dot_general(
        jnp.where(pick, 1.0, 0.0).astype(bf16), full[...], (((1,), (1,)), ((), ())),
        preferred_element_type=f32,
    ).astype(bf16)
    right_sum = jnp.dot(own_columns, full[...], preferred_element_type=f32)
    rnew[0] = decay_rate * rstatb[...] + (1.0 - decay_rate) * (right_sum / width)
    for k in range(1, ntp):
        b = t ^ k
        remote(tpred.at[b], tpred.at[b], rts.at[k], rtr.at[b], f, b).wait_recv()
    fsred[f] = jnp.sum(tpred[...], axis=0)

    def fs_red(k):
        peer = lax.rem(f + k + 1, nfs)
        return remote(fsred.at[f], fsred.at[f], rfs.at[k], rfr.at[f], peer, t)

    loop(nfs - 1, lambda k: fs_red(k).start())

    outer = lax.dot_general(
        full[chunk(f), :], full[...], (((1,), (1,)), ((), ())), preferred_element_type=f32
    )
    lnew[0] = decay_rate * lstatb[...] + (1.0 - decay_rate) * (outer / chans)

    def fs_take(k):
        peer = lax.rem(f + k + 1, nfs)
        remote(fsred.at[peer], fsred.at[peer], rfs.at[k], rfr.at[peer], peer, t).wait_recv()

    loop(nfs - 1, fs_take)
    totals = jnp.sum(fsred[...], axis=0)
    scale = jnp.sqrt(totals[0:1, 0:1] + 1.0) / jnp.sqrt(totals[1:2, 0:1] + 1.0)
    stepv = scale * step[...]
    step[...] = stepv
    new = wb[...] - step_size * stepv
    new_w[...] = new
    wcopy[chunk(f), :] = new.astype(bf16)
    wa = (wcopy, wzs, wzr, wys, wyr)
    gather_start(wa)

    for p in range(pieces):
        for k in far:
            own_copy(k, p).wait_send()
            forward_copy(k, p).wait_send()
        if ntp > 1:
            own_copy(1, p).wait_send()
    for s in range(ntp):
        y_copy(s).wait_send()

    def z_drain(k):
        z_copy(lax.rem(z + k + 1, nz)).wait_send()

    loop(nz - 1, z_drain)
    gather_drain(ga)
    for k in range(1, ntp):
        tp_red(k).wait_send()
    loop(nfs - 1, lambda k: fs_red(k).wait_send())

    gather_relay(wa)
    loop(nz, functools.partial(gather_pair, wa))
    gather_drain(wa)


def body(nfs, ntp, rnn_out, out_grad, weight, left_root, right_root, left_stat, right_stat):
    rows, chans = weight.shape
    tokens, dl = out_grad.shape
    width = left_root.shape[2]
    rr = right_stat.shape[1]
    nz = nfs // 2
    half = dl // rows // 2
    pieces = 2 if (half == 1 and rows % 128 == 0) else 1
    np_ = 4 if rows % 64 == 0 else 1
    dma = pltpu.SemaphoreType.DMA
    hbm = pl.BlockSpec(memory_space=pl.ANY)
    V = pltpu.VMEM
    return pl.pallas_call(
        functools.partial(kernel, nfs, ntp),
        out_shape=(
            V(weight.shape, f32),
            V(weight.shape, f32),
            V(left_stat.shape, f32),
            V(right_stat.shape, f32),
            V((width, chans), bf16),
        ),
        in_specs=[hbm] * 7,
        out_specs=(pl.BlockSpec(memory_space=V),) * 5,
        scratch_shapes=[
            V((ntp, tokens, dl), bf16),
            V((tokens, chans), bf16),
            V((rows, chans), f32),
            V((rows, width), bf16),
            V((chans, chans), bf16),
            V((rows, width), f32),
            V((rr, chans), f32),
            V((ntp, half, rows, chans), f32),
            V((ntp, half, rows, chans), bf16),
            V((ntp, half, rows, chans), bf16),
            V((nz, rows, chans), bf16),
            V((nz, rows, chans), bf16),
            V((rows, chans), f32),
            V((width, chans), bf16),
            V((ntp, 8, 128), f32),
            V((nfs, 8, 128), f32),
            dma((7,)),
            dma((2 * ntp, pieces)),
            dma((ntp, pieces)),
            dma((ntp,)),
            dma((ntp,)),
            dma((nz,)),
            dma((nz,)),
            dma((2, nz * np_)), dma((nz * np_,)), dma((nz * np_,)), dma((nz * np_,)),
            dma((2, nz * np_)), dma((nz * np_,)), dma((nz * np_,)), dma((nz * np_,)),
            dma((ntp,)), dma((ntp,)),
            dma((nfs,)), dma((nfs,)),
        ],
        compiler_params=pltpu.CompilerParams(
            collective_id=0, has_side_effects=True, vmem_limit_bytes=60000 * 1024
        ),
    )(out_grad, rnn_out, weight, left_root, right_root, left_stat, right_stat)


def solution(mesh):
    placed = (
        P("fs", "tp"),
        P("fs", "tp"),
        P("fs", "tp"),
        P("tp", "fs", None),
        P("tp", None, None),
        P("tp", "fs", None),
        P("tp", "fs", None),
    )
    return jax.shard_map(
        functools.partial(body, mesh.shape["fs"], mesh.shape["tp"]),
        mesh=mesh,
        in_specs=placed,
        out_specs=(
            P("fs", "tp"),
            P("fs", "tp"),
            P("tp", "fs", None),
            P("tp", "fs", None),
            P(None, "tp"),
        ),
        check_vma=False,
    )
```
